32 devices in a mesh: sp: 8 (over z, core), tp: 4 (over y, x).
Axes of the slice: x: 2, y: 2, z: 4, core: 2. Of those that a mesh axis runs over, the one named last changes fastest.
Arguments:
- residual_in: bfloat16 [2048, 2048], P('sp'), may hold values from -6 to 6
- queries: bfloat16 [2048, 2048], P('sp', 'tp'), may hold values from -6 to 4
- keys: bfloat16 [2048, 2048], P('sp', 'tp'), may hold values from -4 to 5.2
- values: bfloat16 [2048, 2048], P('sp', 'tp'), may hold values from -9.5 to 9.5
- out_weight: bfloat16 [2048, 2048], P('tp'), may hold values from -0.125 to 0.125
- norm_gain: float32 [2048], replicated, may hold values from 0.1 to 1.9
- expert_routes: int32 [2048, 2], P('sp'), may hold values from 0 to 7, all different within a row; in each aligned block of 256 rows (0 to 255, 256 to 511, ...) at most 128 rows name the same one
- route_scores: float32 [2048, 2], P('sp'), may hold values from -6 to 6
- gate_weight: bfloat16 [8, 2048, 4096], P('sp', None, 'tp'), may hold values from -0.125 to 0.125
- up_weight: bfloat16 [8, 2048, 4096], P('sp', None, 'tp'), may hold values from -0.125 to 0.125
- down_weight: bfloat16 [8, 4096, 2048], P('sp', 'tp'), may hold values from -0.09375 to 0.09375
Outputs:
- layer_out: bfloat16 [2048, 2048], P('sp', 'tp')
The draws below stay inside these ranges and needn't reach their ends.
Inputs may be any that keep to these rules, and one draw needn't show every extreme that they name: `expert_routes`: each row names 2 different experts; among the 256 rows of one index of sp no expert is named more than 128 times, and in every draw some such block names some expert exactly 128 times.
All inputs are finite; a program needn't handle non-finite values.
Results may differ from the reference program's by a relative error of at most 0.015.
Values may be sent and summed in bfloat16 or wider, within the bound.
A program may use at most 64 MiB of HBM per device.

```python
import math
from functools import partial
import jax
import jax.numpy as jnp
import numpy as np
from jax import lax

D = 2048
HEADS = 32
HD = 64
FF = 4096
TOP = 2
TOKENS_PER_SHARD = 256
SEQUENCE_LENGTH = 2048
EXPERTS = 8
CAP = 128
N_SP = 8
N_TP = 4


def draw_queries(key, part):
    key_fast, jitter_key = jax.random.split(jax.random.fold_in(key, 11))
    slow_mean = -(jnp.log(jnp.float32(SEQUENCE_LENGTH)) + 2.0) / math.sqrt(HD)
    fast_mean = -5.5 / math.sqrt(HD)
    fast = jax.random.bernoulli(key_fast, 0.5, (HEADS,))
    noise = jnp.clip(jax.random.normal(jitter_key, (SEQUENCE_LENGTH, HEADS, HD), jnp.float32), -4.0, 4.0)
    center_values = jnp.where(fast, fast_mean, slow_mean)
    return (center_values[None, :, None] + noise).reshape(SEQUENCE_LENGTH, HEADS * HD).astype(jnp.bfloat16)


def draw_keys(key, part):
    baseline_key, spike_key, jitter_key = jax.random.split(jax.random.fold_in(key, 23), 3)
    baseline_level = jax.random.uniform(baseline_key, (SEQUENCE_LENGTH // TOKENS_PER_SHARD,), jnp.float32, 0.9, 1.1)
    spike_positions = jax.random.randint(spike_key, (8,), 0, SEQUENCE_LENGTH)
    spike_pattern = jnp.zeros((SEQUENCE_LENGTH,), jnp.float32).at[spike_positions].set(1.0)
    center_values = jnp.repeat(baseline_level, TOKENS_PER_SHARD) * (1.0 - spike_pattern)
    noise = jnp.clip(jax.random.normal(jitter_key, (SEQUENCE_LENGTH, HEADS * HD), jnp.float32), -4.0, 4.0)
    return (center_values[:, None] + noise).astype(jnp.bfloat16)


def draw_values(key, part):
    key_offset = jax.random.fold_in(jax.random.fold_in(key, 37), 0)
    jitter_key = jax.random.fold_in(jax.random.fold_in(key, 37), 2)
    offset = jnp.clip(2.0 * jax.random.normal(key_offset, (SEQUENCE_LENGTH // TOKENS_PER_SHARD, HEADS * HD), jnp.float32), -5.0, 5.0)
    noise = jnp.clip(jax.random.normal(jitter_key, (SEQUENCE_LENGTH, HEADS * HD), jnp.float32), -4.0, 4.0)
    return (jnp.repeat(offset, TOKENS_PER_SHARD, axis=0) + noise).astype(jnp.bfloat16)


def block_scale(key, shape, shards, low, top_value):
    def one(dim, shards_of):
        heights = jax.random.uniform(jax.random.fold_in(jax.random.fold_in(key, 6), dim), (shards_of,), jnp.float32, low / len(shards), top_value / len(shards))
        return jnp.repeat(jnp.exp(heights), shape[dim] // shards_of).reshape((-1,) + (1,) * (len(shape) - dim - 1))

    factor_of = one(*shards[0])
    for cut in shards[1:]:
        factor_of = factor_of * one(*cut)
    return factor_of


def deal_out(rng, own, number, rows, count, top, most, skew):
    ranking = jax.random.permutation(rng, count)
    packed, usual = load_shares(count, rows * top, most, skew, True), load_shares(count, rows * top, most, skew, False)
    places = jnp.arange(count)

    def named(sizes, rotation):
        used = int((sizes > 0).sum())
        fixed = max(1, used // 4)
        passed = fixed + (places - fixed + rotation * (used - fixed)) % max(1, count - fixed)
        return jnp.zeros((count,), jnp.int32).at[ranking[jnp.where(places < fixed, places, passed)]].set(jnp.asarray(sizes, jnp.int32))

    sizes = jnp.where(number % 4 == 0, named(packed, number // 4), named(usual, number - number // 4 - 1))
    mixed = jax.random.permutation(jax.random.fold_in(own, 3), count)
    giver, sink = mixed[0:count // 2 * 2:2], mixed[1:count // 2 * 2:2]
    room = jnp.minimum(sizes[giver] - 1, most - sizes[sink]) // 2
    room = jnp.where((giver == ranking[0]) | (sink == ranking[0]) | (sizes[sink] == 0), 0, jnp.maximum(room, 0))
    passed = jax.random.randint(jax.random.fold_in(own, 4), (count // 2,), 0, 1 << 20) % (room + 1)
    sizes = sizes.at[giver].add(-passed).at[sink].add(passed)
    items = jnp.searchsorted(jnp.cumsum(sizes), jnp.arange(rows * top), side="right").astype(jnp.int32)
    listing = items.reshape(top, rows).T
    listing = listing[jax.random.permutation(jax.random.fold_in(own, 1), rows)]
    rotation = jax.random.randint(jax.random.fold_in(own, 2), (rows, 1), 0, top)
    return jnp.take_along_axis(listing, (jnp.arange(top)[None, :] + rotation) % top, axis=1)


def load_shares(count, total, bound, skew, full):
    loads = [(1 << 20) // math.isqrt(rank ** skew) + 1 for rank in range(1, count + 1)]
    largest = bound if full else min(bound, max(-(-total // count), total * loads[0] // sum(loads)))
    least = 1 if total - largest >= count - 1 else 0
    given, spare = [largest] + [least] * (count - 1), total - largest - least * (count - 1)
    while spare > 0:
        free = [i for i in range(1, count) if given[i] < largest] or [i for i in range(1, count) if given[i] < bound]
        mass, budget = sum([loads[i] for i in free]), spare
        for i in free:
            addition = min(bound - given[i], max(1, budget * loads[i] // mass), spare)
            given[i] = given[i] + addition
            spare = spare - addition
    return np.array(given)


def normal_values(stream_key, shape, spread, limit, cuts=(), held_as=jnp.bfloat16):
    entries = jax.random.normal(stream_key, shape, jnp.float32) * spread
    if len(cuts) > 0:
        entries = block_scale(stream_key, shape, cuts, -0.22, 0.18) * entries
    return jnp.clip(entries, min=-limit, max=limit).astype(held_as)


def setup_inputs(seed: int = 0) -> dict:
    streams_of = jax.random.split(jax.random.key(seed), 12)
    residual_in = normal_values(streams_of[0], (SEQUENCE_LENGTH, D), 1.0, 6.0, ((0, 8),))
    queries = draw_queries(jax.random.fold_in(streams_of[11], 71), 0)
    keys = draw_keys(jax.random.fold_in(streams_of[11], 71), 0)
    values = draw_values(jax.random.fold_in(streams_of[11], 71), 0)
    out_weight = normal_values(streams_of[4], (HEADS * HD, D), (HEADS * HD) ** -0.5, 0.125, ((0, 4),))
    norm_gain = jnp.clip(1.0 + 0.18 * jax.random.normal(streams_of[5], (D,), jnp.float32), 0.1, 1.9)
    expert_routes_keys = jax.random.split(jax.random.fold_in(streams_of[6], 1), SEQUENCE_LENGTH // TOKENS_PER_SHARD)
    expert_routes_turns = jax.random.permutation(jax.random.fold_in(streams_of[6], 3), SEQUENCE_LENGTH // TOKENS_PER_SHARD)
    expert_routes = jax.vmap(lambda own, number: deal_out(jax.random.fold_in(streams_of[6], 2), own, number, TOKENS_PER_SHARD, EXPERTS, TOP, CAP, 2))(expert_routes_keys, expert_routes_turns).reshape((SEQUENCE_LENGTH, TOP))
    route_scores = normal_values(streams_of[7], (SEQUENCE_LENGTH, TOP), 1.5, 6.0, ((0, 8),), jnp.float32)
    gate_weight = normal_values(streams_of[8], (EXPERTS, D, FF), D ** -0.5, 0.125, ((0, 8), (2, 4)))
    up_weight = normal_values(streams_of[9], (EXPERTS, D, FF), D ** -0.5, 0.125, ((0, 8), (2, 4)))
    down_weight = normal_values(streams_of[10], (EXPERTS, FF, D), FF ** -0.5, 0.09375, ((0, 8), (1, 4)))
    return dict(residual_in=residual_in, queries=queries, keys=keys, values=values, out_weight=out_weight, norm_gain=norm_gain, expert_routes=expert_routes, route_scores=route_scores, gate_weight=gate_weight, up_weight=up_weight, down_weight=down_weight)


epsilon = 1e-06

def rounded_groups(left, right, groups):
    width = left.shape[1] // groups

    def add_group(total, group_index):
        part_left = lax.dynamic_slice_in_dim(left, group_index * width, width, 1)
        part_right = lax.dynamic_slice_in_dim(right, group_index * width, width, 0)
        term = jnp.dot(part_left, part_right, preferred_element_type=jnp.float32).astype(jnp.bfloat16)
        term = lax.optimization_barrier(term)
        return (total + term.astype(jnp.float32), None)
    start_total = jnp.zeros((left.shape[0], right.shape[1]), jnp.float32)
    total, unused = lax.scan(add_group, start_total, jnp.arange(groups, dtype=jnp.int32))
    return total

def stick_attention(queries, keys, values):
    total_len = queries.shape[0]
    span = min(512, total_len)
    scale = HD ** (-0.5)
    q_heads = queries.reshape(total_len, HEADS, HD).transpose(1, 0, 2)
    k_heads = keys.reshape(total_len, HEADS, HD).transpose(1, 0, 2)
    v_heads = values.reshape(total_len, HEADS, HD).transpose(1, 0, 2)
    pieces = []
    for block_start in range(0, total_len, span):
        block_stop = block_start + span
        query_pos = block_start + jnp.arange(span, dtype=jnp.int32)
        key_pos = jnp.arange(block_stop, dtype=jnp.int32)
        causal = key_pos[None, :] < query_pos[:, None]

        def one_head(operands):
            q_part, k_part, v_part = operands
            scores = jnp.dot(q_part, k_part.T, preferred_element_type=jnp.float32) * scale
            log_keep = jnp.where(causal, jax.nn.log_sigmoid(-scores), 0.0)
            between = lax.cumsum(log_keep, axis=1, reverse=True) - log_keep
            weights = jnp.where(causal, jnp.exp(jax.nn.log_sigmoid(scores) + between), 0.0).astype(jnp.bfloat16)
            return jnp.dot(weights, v_part, preferred_element_type=jnp.float32)
        pieces.append(lax.map(one_head, (q_heads[:, block_start:block_stop], k_heads[:, :block_stop], v_heads[:, :block_stop])))
    joined = jnp.concatenate(pieces, axis=1)
    return joined.transpose(1, 0, 2).reshape(total_len, HEADS * HD).astype(jnp.bfloat16)

def route_targets(routes, experts, capacity):
    flat_routes = routes.reshape(-1)
    onehot = (flat_routes[:, None] == jnp.arange(experts, dtype=jnp.int32)[None, :]).astype(jnp.int32)
    before = jnp.cumsum(onehot, axis=0) - onehot
    return flat_routes * capacity + lax.optimization_barrier(jnp.sum(before * onehot, axis=1))

def run_expert(operands):
    rows_in, gate_part, up_part, down_part = operands
    gate_act = jnp.dot(rows_in, gate_part, preferred_element_type=jnp.float32)
    up_act = jnp.dot(rows_in, up_part, preferred_element_type=jnp.float32)
    hidden = (jax.nn.silu(gate_act) * up_act).astype(jnp.bfloat16)
    return rounded_groups(hidden, down_part, N_TP).astype(jnp.bfloat16)

def reference(residual_in, queries, keys, values, out_weight, norm_gain, expert_routes, route_scores, gate_weight, up_weight, down_weight):
    mixed_heads = stick_attention(queries, keys, values)
    attended = rounded_groups(mixed_heads, out_weight, N_TP).astype(jnp.bfloat16)
    stream = (residual_in.astype(jnp.float32) + attended.astype(jnp.float32)).astype(jnp.bfloat16)
    stream_wide = stream.astype(jnp.float32)
    normed = (stream_wide * lax.rsqrt(lax.optimization_barrier(jnp.mean(stream_wide * stream_wide, axis=1, keepdims=True)) + epsilon) * norm_gain).astype(jnp.bfloat16)
    block_targets = jax.vmap(partial(route_targets, experts=EXPERTS, capacity=CAP))(expert_routes.reshape(N_SP, TOKENS_PER_SHARD, TOP))
    block_ids = jnp.arange(N_SP, dtype=jnp.int32)[:, None]
    global_slots = block_targets // CAP * (N_SP * CAP) + block_ids * CAP + block_targets % CAP
    owners = block_ids * TOKENS_PER_SHARD + jnp.arange(TOKENS_PER_SHARD * TOP, dtype=jnp.int32)[None, :] // TOP
    slot_owner = jnp.full((EXPERTS * N_SP * CAP,), SEQUENCE_LENGTH, jnp.int32).at[global_slots.reshape(-1)].set(owners.reshape(-1))
    padded = jnp.concatenate([normed, jnp.zeros((1, D), jnp.bfloat16)], axis=0)
    gathered = padded[slot_owner].reshape(EXPERTS, N_SP * CAP, D)
    outputs = lax.map(run_expert, (gathered, gate_weight, up_weight, down_weight))
    results = outputs.reshape(EXPERTS * N_SP * CAP, D)
    picked = results[global_slots.reshape(-1)].astype(jnp.float32).reshape(SEQUENCE_LENGTH, TOP, D)
    shares = jax.nn.sigmoid(route_scores - route_scores[:, ::-1])
    combined = lax.optimization_barrier(jnp.sum(picked * shares[:, :, None], axis=1))
    return (stream_wide + combined).astype(jnp.bfloat16)
```

```python
import functools

import jax
import jax.numpy as jnp
from jax import lax
from jax.experimental import pallas as pl
from jax.experimental.pallas import tpu as pltpu
from jax.sharding import PartitionSpec as P

HD = 64


epsilon = 1e-06


def attend(queries, query_start, keys_all, values_all):
    row_count = queries.shape[0]
    total_len = keys_all.shape[0]
    head_count = queries.shape[1] // HD
    span = min(512, total_len)
    scale = HD ** (-0.5)
    query_heads = queries.reshape(row_count, head_count, HD)
    query_pos = query_start + lax.iota(jnp.int32, row_count)
    block_count = (query_start + row_count - 1 + span - 1) // span

    def one_block(step_index, state_pair):
        accumulated, kept_log = state_pair
        key_start = (block_count - 1 - step_index) * span
        key_block = lax.dynamic_slice_in_dim(keys_all, key_start, span, 0).reshape(
            span, head_count, HD
        )
        value_block = lax.dynamic_slice_in_dim(values_all, key_start, span, 0).reshape(
            span, head_count, HD
        )
        scores = (
            jnp.einsum("qhc,khc->hqk", query_heads, key_block, preferred_element_type=jnp.float32)
            * scale
        )
        key_pos = key_start + lax.iota(jnp.int32, span)
        causal = key_pos[None, :] < query_pos[:, None]
        log_keep = jnp.where(causal, jax.nn.log_sigmoid(-scores), 0.0)
        between = lax.cumsum(log_keep, axis=2, reverse=True) - log_keep + kept_log[:, :, None]
        weights = jnp.where(causal, jnp.exp(jax.nn.log_sigmoid(scores) + between), 0.0).astype(
            jnp.bfloat16
        )
        accumulated = accumulated + jnp.einsum(
            "hqk,khc->qhc", weights, value_block, preferred_element_type=jnp.float32
        )
        return (accumulated, kept_log + jnp.sum(log_keep, axis=2))

    start_pair = (
        jnp.zeros((row_count, head_count, HD), jnp.float32),
        jnp.zeros((head_count, row_count), jnp.float32),
    )
    accumulated, kept_log = lax.fori_loop(0, block_count, one_block, start_pair)
    return accumulated.reshape(row_count, head_count * HD).astype(jnp.bfloat16)


def route_targets(routes, experts, capacity):
    flat_routes = routes.reshape(-1)
    onehot = (flat_routes[:, None] == lax.iota(jnp.int32, experts)[None, :]).astype(jnp.int32)
    before = jnp.cumsum(onehot, axis=0) - onehot
    return flat_routes * capacity + jnp.sum(before * onehot, axis=1)


def shards(
    residual_in,
    queries,
    keys,
    values,
    out_weight,
    norm_gain,
    expert_routes,
    route_scores,
    gate_weight,
    up_weight,
    down_weight,
):
    row_count = residual_in.shape[0]
    width = residual_in.shape[1]
    row_start = lax.axis_index("sp") * row_count
    keys_all, values_all = (
        lax.all_gather(keys, "sp", axis=0, tiled=True),
        lax.all_gather(values, "sp", axis=0, tiled=True),
    )
    mixed_heads = attend(queries, row_start, keys_all, values_all)
    partial_value = jnp.dot(mixed_heads, out_weight, preferred_element_type=jnp.float32).astype(
        jnp.bfloat16
    )
    attended = lax.psum(partial_value, "tp").astype(jnp.float32).astype(jnp.bfloat16)
    stream = (residual_in.astype(jnp.float32) + attended.astype(jnp.float32)).astype(jnp.bfloat16)
    stream_wide = stream.astype(jnp.float32)
    normed = (
        stream_wide
        * lax.rsqrt(jnp.mean(stream_wide * stream_wide, axis=1, keepdims=True) + epsilon)
        * norm_gain
    ).astype(jnp.bfloat16)
    experts = lax.axis_size("sp")
    capacity = 4 * row_count // experts
    top_count = expert_routes.shape[1]
    targets = route_targets(expert_routes, experts, capacity)
    owners = lax.iota(jnp.int32, row_count * top_count) // top_count
    slot_owner = jnp.full((experts * capacity,), row_count, jnp.int32).at[targets].set(owners)
    padded = jnp.concatenate([normed, jnp.zeros((1, width), jnp.bfloat16)], axis=0)
    outgoing = padded[slot_owner].reshape(experts, capacity, width)
    col_count = width // lax.axis_size("tp")
    column_start = lax.axis_index("tp") * col_count
    own_part = lax.dynamic_slice_in_dim(outgoing, column_start, col_count, 2)
    arrived = lax.all_to_all(own_part, "sp", split_axis=0, concat_axis=0, tiled=True)
    arrived = lax.all_gather(arrived, "tp", axis=2, tiled=True)
    slot_rows = arrived.reshape(-1, width)
    gate_act = jnp.dot(slot_rows, gate_weight[0], preferred_element_type=jnp.float32)
    up_act = jnp.dot(slot_rows, up_weight[0], preferred_element_type=jnp.float32)
    hidden = (jax.nn.silu(gate_act) * up_act).astype(jnp.bfloat16)
    expert_part = (
        jnp.dot(hidden, down_weight[0], preferred_element_type=jnp.float32)
        .astype(jnp.bfloat16)
        .reshape(arrived.shape)
    )
    summed = (
        lax.psum_scatter(expert_part, "tp", scatter_dimension=2, tiled=True)
        .astype(jnp.float32)
        .astype(jnp.bfloat16)
    )
    returned = lax.all_to_all(summed, "sp", split_axis=0, concat_axis=0, tiled=True)
    results = returned.reshape(experts * capacity, col_count)
    picked = results[targets].astype(jnp.float32).reshape(row_count, top_count, col_count)
    shares = jax.nn.sigmoid(route_scores - route_scores[:, ::-1])
    combined = jnp.sum(picked * shares[:, :, None], axis=1)
    own_columns = lax.dynamic_slice_in_dim(stream_wide, column_start, col_count, 1)
    return (own_columns + combined).astype(jnp.bfloat16)


F32 = jnp.float32
BF16 = jnp.bfloat16
MESH = pl.DeviceIdType.MESH
VM = pl.BlockSpec(memory_space=pltpu.VMEM)


def dot_f32(left, right, left_dim=1, right_dim=0):
    return lax.dot_general(
        left, right, (((left_dim,), (right_dim,)), ((), ())), preferred_element_type=F32
    )


def greet(peers):
    barrier = pltpu.get_barrier_semaphore()
    for peer in peers:
        pl.semaphore_signal(barrier, inc=1, device_id=peer, device_id_type=MESH)
    pl.semaphore_wait(barrier, len(peers))


def attention_kernel(
    n, q_ref, k_ref, v_ref, out_ref, pack, recv, made, back, send1, recv1, send2, recv2
):
    me = lax.axis_index("sp")
    block = q_ref.shape[0]

    def outward(dst, slot, src):
        return pltpu.make_async_remote_copy(
            src_ref=pack.at[dst],
            dst_ref=recv.at[src],
            send_sem=send1.at[slot],
            recv_sem=recv1.at[src],
            device_id={"sp": dst},
            device_id_type=MESH,
        )

    def homeward(dst, src):
        return pltpu.make_async_remote_copy(
            src_ref=made.at[dst],
            dst_ref=back.at[src],
            send_sem=send2.at[dst],
            recv_sem=recv2.at[src],
            device_id={"sp": dst},
            device_id_type=MESH,
        )

    scaled = (q_ref[...].astype(F32) * HD ** (-0.5)).astype(BF16)
    for place, array in enumerate((scaled, k_ref[...], v_ref[...])):
        turned = array.T
        for h in range(n):
            pack[h, place * HD : (place + 1) * HD, :] = turned[h * HD : (h + 1) * HD, :]
    others = [lax.rem(me + d, n) for d in range(1, n)]
    greet([{"sp": p} for p in others])
    for d, dst in enumerate(others):
        outward(dst, d, me).start()
    recv[me] = pack[me]

    rows = lax.broadcasted_iota(jnp.int32, (block, block), 0)
    cols = lax.broadcasted_iota(jnp.int32, (block, block), 1)
    upper = (cols >= rows).astype(F32).astype(BF16)
    causal = rows < cols

    def one(i, j, acc, kept, diagonal):
        q_t = recv[i, 0:HD, :]
        k_t = recv[j, HD : 2 * HD, :]
        v_t = recv[j, 2 * HD : 3 * HD, :]
        z = dot_f32(k_t, q_t, 0, 0)
        drop = jnp.maximum(z, 0.0) + jnp.log(1.0 + jnp.exp(-jnp.abs(z)))
        if diagonal:
            drop = jnp.where(causal, drop, 0.0)
        high = drop.astype(BF16)
        low = (drop - high.astype(F32)).astype(BF16)
        total = dot_f32(upper, high) + dot_f32(upper, low)
        w = jnp.exp(z - total - kept)
        if diagonal:
            w = jnp.where(causal, w, 0.0)
        acc = acc + dot_f32(v_t, w.astype(BF16))
        return acc, kept + total[0:1, :]

    for i in range(n):

        @pl.when(me != i)
        def _():
            outward(i, 0, i).wait_recv()

        acc = jnp.zeros((HD, block), F32)
        kept = jnp.zeros((1, block), F32)
        acc, kept = one(i, i, acc, kept, True)
        acc, kept = lax.fori_loop(
            0, i, lambda step, state: one(i, i - 1 - step, state[0], state[1], False), (acc, kept)
        )
        made[i] = acc.astype(BF16)

        @pl.when(me != i)
        def _():
            homeward(i, me).start()

    back[me] = made[me]
    for d, dst in enumerate(others):
        outward(dst, d, me).wait_send()
        homeward(dst, dst).wait()
    out_ref[...] = back[...]


def attend_by_head(n, queries, keys, values):
    block = queries.shape[0]
    return pl.pallas_call(
        functools.partial(attention_kernel, n),
        out_shape=jax.ShapeDtypeStruct((n, HD, block), BF16),
        in_specs=[VM] * 3,
        out_specs=VM,
        scratch_shapes=[
            pltpu.VMEM((n, 3 * HD, block), BF16),
            pltpu.VMEM((n, 3 * HD, block), BF16),
            pltpu.VMEM((n, HD, block), BF16),
            pltpu.VMEM((n, HD, block), BF16),
            pltpu.SemaphoreType.DMA((n,)),
            pltpu.SemaphoreType.DMA((n,)),
            pltpu.SemaphoreType.DMA((n,)),
            pltpu.SemaphoreType.DMA((n,)),
        ],
        compiler_params=pltpu.CompilerParams(collective_id=0, has_side_effects=True),
    )(queries, keys, values)


def expert_kernel(
    n_sp,
    n_tp,
    mixed_ref,
    ow_ref,
    res_ref,
    gain_ref,
    tgt_rows_ref,
    tgt_cols_ref,
    share_ref,
    gate_hbm,
    up_hbm,
    down_hbm,
    out_ref,
    gate_w,
    up_w,
    down_w,
    terms,
    terms_in,
    sums,
    sums_in,
    outgoing,
    arrived,
    hidden,
    parts,
    parts_in,
    ret,
    ret_in,
    stream_s,
    w_sem,
    s_term,
    r_term,
    s_sum,
    r_sum,
    s_out,
    r_out,
    s_ag,
    r_ag,
    s_part,
    r_part,
    s_ret,
    r_ret,
):
    s, t = lax.axis_index("sp"), lax.axis_index("tp")
    rows, col = stream_s.shape
    width = col * n_tp
    cap = outgoing.shape[0] // n_sp
    groups = n_sp // 2
    span = 2 * cap
    sp_others = [lax.rem(s + d, n_sp) for d in range(1, n_sp)]
    tp_others = [lax.rem(t + d, n_tp) for d in range(1, n_tp)]
    loads = [
        pltpu.make_async_copy(a, b, w_sem.at[i])
        for i, (a, b) in enumerate(((gate_hbm, gate_w), (up_hbm, up_w), (down_hbm, down_w)))
    ]
    for load in loads:
        load.start()

    def remote(src, dst, send, recv, device):
        return pltpu.make_async_remote_copy(
            src_ref=src,
            dst_ref=dst,
            send_sem=send,
            recv_sem=recv,
            device_id=device,
            device_id_type=MESH,
        )

    def term_copy(d):
        return remote(
            terms.at[d], terms_in.at[d], s_term.at[d], r_term.at[d], {"tp": tp_others[d]}
        )

    def sum_copy(d):
        return remote(sums, sums_in.at[d], s_sum.at[d], r_sum.at[d], {"tp": tp_others[d]})

    def at(start, size):
        return pl.ds(pl.multiple_of(start, size), size)

    def out_copy(dst, src):
        return remote(
            outgoing.at[at(dst * cap, cap)],
            arrived.at[t, at(src * cap, cap)],
            s_out.at[dst],
            r_out.at[src],
            {"sp": dst},
        )

    def ag_copy(d, g):
        piece = arrived.at[t, at(g * span, span)]
        return remote(piece, piece, s_ag.at[d, g], r_ag.at[d, g], {"tp": tp_others[d]})

    def ag_wait(d, g):
        piece = arrived.at[lax.rem(t + n_tp - 1 - d, n_tp), at(g * span, span)]
        remote(piece, piece, s_ag.at[d, g], r_ag.at[d, g], {"tp": tp_others[d]}).wait_recv()

    def part_copy(d, g):
        return remote(
            parts.at[d, at(g * span, span)],
            parts_in.at[d, at(g * span, span)],
            s_part.at[d, g],
            r_part.at[d, g],
            {"tp": tp_others[d]},
        )

    def ret_copy(dst, src):
        return remote(
            ret.at[at(dst * cap, cap)],
            ret_in.at[at(src * cap, cap)],
            s_ret.at[dst],
            r_ret.at[src],
            {"sp": dst},
        )

    greet([{"tp": p} for p in tp_others] + [{"sp": p} for p in sp_others])
    mixed = mixed_ref[...].T
    for d in range(n_tp - 1):
        terms[d] = dot_f32(mixed, ow_ref[:, at(tp_others[d] * col, col)]).astype(BF16)
        term_copy(d).start()
    attended = dot_f32(mixed, ow_ref[:, at(t * col, col)]).astype(BF16).astype(F32)
    for d in range(n_tp - 1):
        term_copy(d).wait_recv()
        attended = attended + terms_in[d].astype(F32)
    attended = attended.astype(BF16).astype(F32)
    stream = (res_ref[:, at(t * col, col)].astype(F32) + attended).astype(BF16).astype(F32)
    stream_s[...] = stream
    squares = jnp.sum(stream * stream, axis=1, keepdims=True)
    sums[...] = jnp.broadcast_to(squares, (rows, 128)).T[0:8, :]
    for d in range(n_tp - 1):
        sum_copy(d).start()
    square_row = sums[0:1, :]
    for d in range(n_tp - 1):
        sum_copy(d).wait_recv()
        square_row = square_row + sums_in[d, 0:1, :]
    squares = jnp.broadcast_to(square_row, (128, rows)).T[:, 0:1]
    normed = (
        stream * lax.rsqrt(squares * (1.0 / width) + epsilon) * gain_ref[0:1, at(t * col, col)]
    ).astype(BF16)
    first, second = tgt_rows_ref[0:1, :], tgt_rows_ref[1:2, :]
    slot_in = lax.broadcasted_iota(jnp.int32, (cap, rows), 0)

    def dispatch(e):
        slots = slot_in + e * cap
        pick = ((first == slots) | (second == slots)).astype(F32).astype(BF16)
        return dot_f32(pick, normed).astype(BF16)

    for dst in sp_others:
        outgoing[at(dst * cap, cap), :] = dispatch(dst)
        out_copy(dst, s).start()
    arrived[t, at(s * cap, cap), :] = dispatch(s)
    for load in loads:
        load.wait()
    chip = s // 2

    def relay(k):
        g = lax.rem(chip + k, groups)
        for core in range(2):
            src = 2 * g + core

            @pl.when(src != s)
            def _():
                out_copy(src, src).wait_recv()

        for d in range(n_tp - 1):
            ag_copy(d, g).start()

    def compute(k):
        g = lax.rem(chip + k, groups)
        for d in range(n_tp - 1):
            ag_wait(d, g)
        ff = gate_w.shape[1]
        tile = min(256, ff)
        here = at(g * span, span)

        def hidden_tile(i, carry):
            lanes = at(i * tile, tile)
            gate_act = jnp.zeros((span, tile), F32)
            up_act = jnp.zeros((span, tile), F32)
            for c in range(n_tp):
                x = arrived[c, here, :]
                gate_act = gate_act + dot_f32(x, gate_w[c * col : (c + 1) * col, lanes])
                up_act = up_act + dot_f32(x, up_w[c * col : (c + 1) * col, lanes])
            act = gate_act / (1.0 + jnp.exp(-gate_act)) * up_act
            hidden[:, lanes] = act.astype(BF16)
            return carry

        lax.fori_loop(0, ff // tile, hidden_tile, 0)
        for d in range(n_tp - 1):
            parts[d, here, :] = dot_f32(
                hidden[...], down_w[:, at(tp_others[d] * col, col)]
            ).astype(BF16)
            part_copy(d, g).start()
        parts[n_tp - 1, here, :] = dot_f32(hidden[...], down_w[:, at(t * col, col)]).astype(BF16)

    def finish(k):
        g = lax.rem(chip + k, groups)
        here = at(g * span, span)
        total = parts[n_tp - 1, here, :].astype(F32)
        for d in range(n_tp - 1):
            part_copy(d, g).wait_recv()
            total = total + parts_in[d, here, :].astype(F32)
        ret[here, :] = total.astype(BF16)
        for core in range(2):
            src = 2 * g + core

            @pl.when(src != s)
            def _():
                ret_copy(src, s).start()

    relay(0)

    def step(k, carry):
        @pl.when(k + 1 < groups)
        def _():
            relay(k + 1)

        compute(k)

        @pl.when(k > 0)
        def _():
            finish(k - 1)

        return carry

    lax.fori_loop(0, groups, step, 0)
    finish(groups - 1)
    ret_in[at(s * cap, cap), :] = ret[at(s * cap, cap), :]
    for dst in sp_others:
        ret_copy(dst, dst).wait_recv()
    slots = lax.broadcasted_iota(jnp.int32, (rows, n_sp * cap), 1)
    total = jnp.zeros((rows, col), F32)
    for k in range(2):
        pick = (tgt_cols_ref[:, k : k + 1] == slots).astype(F32).astype(BF16)
        other = share_ref[:, 1 - k : 2 - k]
        share = 1.0 / (1.0 + jnp.exp(other - share_ref[:, k : k + 1]))
        total = total + dot_f32(pick, ret_in[...]) * share
    out_ref[...] = (stream_s[...] + total).astype(BF16)
    for d in range(n_tp - 1):
        term_copy(d).wait_send()
        sum_copy(d).wait_send()
    for dst in sp_others:
        out_copy(dst, s).wait_send()
        ret_copy(dst, s).wait_send()

    def drain(g, carry):
        for d in range(n_tp - 1):
            ag_copy(d, g).wait_send()
            part_copy(d, g).wait_send()
        return carry

    lax.fori_loop(0, groups, drain, 0)


def fused_shards(
    n_sp,
    n_tp,
    residual_in,
    queries,
    keys,
    values,
    out_weight,
    norm_gain,
    expert_routes,
    route_scores,
    gate_weight,
    up_weight,
    down_weight,
):
    rows, width = residual_in.shape
    col = width // n_tp
    cap = 4 * rows // n_sp
    slots = n_sp * cap
    ff = gate_weight.shape[2]
    mixed = attend_by_head(n_sp, queries, keys, values).reshape(n_sp * HD, rows)
    targets = route_targets(expert_routes, n_sp, cap).reshape(rows, 2)
    anywhere = pl.BlockSpec(memory_space=pl.ANY)
    dma = pltpu.SemaphoreType.DMA
    far = n_tp - 1
    groups = n_sp // 2
    return pl.pallas_call(
        functools.partial(expert_kernel, n_sp, n_tp),
        out_shape=jax.ShapeDtypeStruct((rows, col), BF16),
        in_specs=[VM] * 7 + [anywhere] * 3,
        out_specs=VM,
        scratch_shapes=[
            pltpu.VMEM((width, ff), BF16),
            pltpu.VMEM((width, ff), BF16),
            pltpu.VMEM((ff, width), BF16),
            pltpu.VMEM((far, rows, col), BF16),
            pltpu.VMEM((far, rows, col), BF16),
            pltpu.VMEM((8, rows), F32),
            pltpu.VMEM((far, 8, rows), F32),
            pltpu.VMEM((slots, col), BF16),
            pltpu.VMEM((n_tp, slots, col), BF16),
            pltpu.VMEM((2 * cap, ff), BF16),
            pltpu.VMEM((n_tp, slots, col), BF16),
            pltpu.VMEM((far, slots, col), BF16),
            pltpu.VMEM((slots, col), BF16),
            pltpu.VMEM((slots, col), BF16),
            pltpu.VMEM((rows, col), F32),
            dma((3,)),
            dma((far,)),
            dma((far,)),
            dma((far,)),
            dma((far,)),
            dma((n_sp,)),
            dma((n_sp,)),
            dma((far, groups)),
            dma((far, groups)),
            dma((far, groups)),
            dma((far, groups)),
            dma((n_sp,)),
            dma((n_sp,)),
        ],
        compiler_params=pltpu.CompilerParams(
            collective_id=1, has_side_effects=True, vmem_limit_bytes=60 * 1024 * 1024
        ),
    )(
        mixed,
        out_weight,
        residual_in,
        norm_gain.reshape(1, width),
        targets.T,
        targets,
        route_scores,
        gate_weight[0],
        up_weight[0],
        down_weight[0],
    )


def solution(mesh):
    in_specs = (
        P("sp", None),
        P("sp", "tp"),
        P("sp", "tp"),
        P("sp", "tp"),
        P("tp", None),
        P(),
        P("sp", None),
        P("sp", None),
        P("sp", None, "tp"),
        P("sp", None, "tp"),
        P("sp", "tp", None),
    )
    out_specs = P("sp", "tp")
    n_sp, n_tp = mesh.shape["sp"], mesh.shape["tp"]

    def body(*args):
        heads = args[1].shape[1] // HD
        if heads == n_sp:
            return fused_shards(n_sp, n_tp, *args)
        return shards(*args)

    return jax.shard_map(body, mesh=mesh, in_specs=in_specs, out_specs=out_specs, check_vma=False)
```

```python
import functools

import jax
import jax.numpy as jnp
from jax import lax
from jax.experimental import pallas as pl
from jax.experimental.pallas import tpu as pltpu
from jax.sharding import PartitionSpec as P

HD = 64


epsilon = 1e-06


def attend(queries, query_start, keys_all, values_all):
    row_count = queries.shape[0]
    total_len = keys_all.shape[0]
    head_count = queries.shape[1] // HD
    span = min(512, total_len)
    scale = HD ** (-0.5)
    query_heads = queries.reshape(row_count, head_count, HD)
    query_pos = query_start + lax.iota(jnp.int32, row_count)
    block_count = (query_start + row_count - 1 + span - 1) // span

    def one_block(step_index, state_pair):
        accumulated, kept_log = state_pair
        key_start = (block_count - 1 - step_index) * span
        key_block = lax.dynamic_slice_in_dim(keys_all, key_start, span, 0).reshape(
            span, head_count, HD
        )
        value_block = lax.dynamic_slice_in_dim(values_all, key_start, span, 0).reshape(
            span, head_count, HD
        )
        scores = (
            jnp.einsum("qhc,khc->hqk", query_heads, key_block, preferred_element_type=jnp.float32)
            * scale
        )
        key_pos = key_start + lax.iota(jnp.int32, span)
        causal = key_pos[None, :] < query_pos[:, None]
        log_keep = jnp.where(causal, jax.nn.log_sigmoid(-scores), 0.0)
        between = lax.cumsum(log_keep, axis=2, reverse=True) - log_keep + kept_log[:, :, None]
        weights = jnp.where(causal, jnp.exp(jax.nn.log_sigmoid(scores) + between), 0.0).astype(
            jnp.bfloat16
        )
        accumulated = accumulated + jnp.einsum(
            "hqk,khc->qhc", weights, value_block, preferred_element_type=jnp.float32
        )
        return (accumulated, kept_log + jnp.sum(log_keep, axis=2))

    start_pair = (
        jnp.zeros((row_count, head_count, HD), jnp.float32),
        jnp.zeros((head_count, row_count), jnp.float32),
    )
    accumulated, kept_log = lax.fori_loop(0, block_count, one_block, start_pair)
    return accumulated.reshape(row_count, head_count * HD).astype(jnp.bfloat16)


def route_targets(routes, experts, capacity):
    flat_routes = routes.reshape(-1)
    onehot = (flat_routes[:, None] == lax.iota(jnp.int32, experts)[None, :]).astype(jnp.int32)
    before = jnp.cumsum(onehot, axis=0) - onehot
    return flat_routes * capacity + jnp.sum(before * onehot, axis=1)


def shards(
    residual_in,
    queries,
    keys,
    values,
    out_weight,
    norm_gain,
    expert_routes,
    route_scores,
    gate_weight,
    up_weight,
    down_weight,
):
    row_count = residual_in.shape[0]
    width = residual_in.shape[1]
    row_start = lax.axis_index("sp") * row_count
    keys_all, values_all = (
        lax.all_gather(keys, "sp", axis=0, tiled=True),
        lax.all_gather(values, "sp", axis=0, tiled=True),
    )
    mixed_heads = attend(queries, row_start, keys_all, values_all)
    partial_value = jnp.dot(mixed_heads, out_weight, preferred_element_type=jnp.float32).astype(
        jnp.bfloat16
    )
    attended = lax.psum(partial_value, "tp").astype(jnp.float32).astype(jnp.bfloat16)
    stream = (residual_in.astype(jnp.float32) + attended.astype(jnp.float32)).astype(jnp.bfloat16)
    stream_wide = stream.astype(jnp.float32)
    normed = (
        stream_wide
        * lax.rsqrt(jnp.mean(stream_wide * stream_wide, axis=1, keepdims=True) + epsilon)
        * norm_gain
    ).astype(jnp.bfloat16)
    experts = lax.axis_size("sp")
    capacity = 4 * row_count // experts
    top_count = expert_routes.shape[1]
    targets = route_targets(expert_routes, experts, capacity)
    owners = lax.iota(jnp.int32, row_count * top_count) // top_count
    slot_owner = jnp.full((experts * capacity,), row_count, jnp.int32).at[targets].set(owners)
    padded = jnp.concatenate([normed, jnp.zeros((1, width), jnp.bfloat16)], axis=0)
    outgoing = padded[slot_owner].reshape(experts, capacity, width)
    col_count = width // lax.axis_size("tp")
    column_start = lax.axis_index("tp") * col_count
    own_part = lax.dynamic_slice_in_dim(outgoing, column_start, col_count, 2)
    arrived = lax.all_to_all(own_part, "sp", split_axis=0, concat_axis=0, tiled=True)
    arrived = lax.all_gather(arrived, "tp", axis=2, tiled=True)
    slot_rows = arrived.reshape(-1, width)
    gate_act = jnp.dot(slot_rows, gate_weight[0], preferred_element_type=jnp.float32)
    up_act = jnp.dot(slot_rows, up_weight[0], preferred_element_type=jnp.float32)
    hidden = (jax.nn.silu(gate_act) * up_act).astype(jnp.bfloat16)
    expert_part = (
        jnp.dot(hidden, down_weight[0], preferred_element_type=jnp.float32)
        .astype(jnp.bfloat16)
        .reshape(arrived.shape)
    )
    summed = (
        lax.psum_scatter(expert_part, "tp", scatter_dimension=2, tiled=True)
        .astype(jnp.float32)
        .astype(jnp.bfloat16)
    )
    returned = lax.all_to_all(summed, "sp", split_axis=0, concat_axis=0, tiled=True)
    results = returned.reshape(experts * capacity, col_count)
    picked = results[targets].astype(jnp.float32).reshape(row_count, top_count, col_count)
    shares = jax.nn.sigmoid(route_scores - route_scores[:, ::-1])
    combined = jnp.sum(picked * shares[:, :, None], axis=1)
    own_columns = lax.dynamic_slice_in_dim(stream_wide, column_start, col_count, 1)
    return (own_columns + combined).astype(jnp.bfloat16)


F32 = jnp.float32
BF16 = jnp.bfloat16
MESH = pl.DeviceIdType.MESH
VM = pl.BlockSpec(memory_space=pltpu.VMEM)


def dot_f32(left, right, left_dim=1, right_dim=0):
    return lax.dot_general(
        left, right, (((left_dim,), (right_dim,)), ((), ())), preferred_element_type=F32
    )


def greet(peers):
    barrier = pltpu.get_barrier_semaphore()
    for peer in peers:
        pl.semaphore_signal(barrier, inc=1, device_id=peer, device_id_type=MESH)
    pl.semaphore_wait(barrier, len(peers))


def attention_kernel(
    n, q_ref, k_ref, v_ref, pack, recv, made, back, send1, recv1, send2, recv2
):
    me = lax.axis_index("sp")
    block = q_ref.shape[0]

    def outward(dst, slot, src):
        return pltpu.make_async_remote_copy(
            src_ref=pack.at[dst],
            dst_ref=recv.at[src],
            send_sem=send1.at[slot],
            recv_sem=recv1.at[src],
            device_id={"sp": dst},
            device_id_type=MESH,
        )

    def homeward(dst, src):
        return pltpu.make_async_remote_copy(
            src_ref=made.at[dst],
            dst_ref=back.at[src],
            send_sem=send2.at[dst],
            recv_sem=recv2.at[src],
            device_id={"sp": dst},
            device_id_type=MESH,
        )

    scaled = (q_ref[...].astype(F32) * HD ** (-0.5)).astype(BF16)
    for place, array in enumerate((scaled, k_ref[...], v_ref[...])):
        turned = array.T
        for h in range(n):
            pack[h, place * HD : (place + 1) * HD, :] = turned[h * HD : (h + 1) * HD, :]
    others = [lax.rem(me + d, n) for d in range(1, n)]
    for d, dst in enumerate(others):
        outward(dst, d, me).start()
    recv[me] = pack[me]

    rows = lax.broadcasted_iota(jnp.int32, (block, block), 0)
    cols = lax.broadcasted_iota(jnp.int32, (block, block), 1)
    upper = (cols >= rows).astype(F32).astype(BF16)
    causal = rows < cols

    def one(i, j, acc, kept, diagonal):
        q_t = recv[i, 0:HD, :]
        k_t = recv[j, HD : 2 * HD, :]
        v_t = recv[j, 2 * HD : 3 * HD, :]
        z = dot_f32(k_t, q_t, 0, 0)
        drop = jnp.maximum(z, 0.0) + jnp.log(1.0 + jnp.exp(-jnp.abs(z)))
        if diagonal:
            drop = jnp.where(causal, drop, 0.0)
        high = drop.astype(BF16)
        low = (drop - high.astype(F32)).astype(BF16)
        total = dot_f32(upper, high) + dot_f32(upper, low)
        w = jnp.exp(z - total - kept)
        if diagonal:
            w = jnp.where(causal, w, 0.0)
        acc = acc + dot_f32(v_t, w.astype(BF16))
        return acc, kept + total[0:1, :]

    for i in range(n):

        @pl.when(me != i)
        def _():
            outward(i, 0, i).wait_recv()

        state = one(i, i, jnp.zeros((HD, block), F32), jnp.zeros((1, block), F32), True)
        odd = i % 2
        if odd:
            state = one(i, i - 1, *state, False)

        def pair(step, state):
            j = i - 1 - odd - 2 * step
            return one(i, j - 1, *one(i, j, *state, False), False)

        state = lax.fori_loop(0, i // 2, pair, state)
        made[i] = state[0].astype(BF16)

        @pl.when(me != i)
        def _():
            homeward(i, me).start()

    back[me] = made[me]
    for d, dst in enumerate(others):
        outward(dst, d, me).wait_send()
        homeward(dst, dst).wait()


def expert_kernel(
    n_sp,
    n_tp,
    q_ref,
    k_ref,
    v_ref,
    routes_ref,
    scores_ref,
    gain_ref,
    ow_hbm,
    res_hbm,
    gate_hbm,
    up_hbm,
    down_hbm,
    out_ref,
    pack,
    recv,
    made,
    back,
    send1,
    recv1,
    send2,
    recv2,
    ow_ref,
    res_ref,
    gate_w,
    up_w,
    down_w,
    terms,
    terms_in,
    sums,
    sums_in,
    outgoing,
    arrived,
    hidden,
    parts,
    mid,
    parts_in,
    ret,
    ret_in,
    stream_s,
    w_sem,
    s_term,
    r_term,
    s_sum,
    r_sum,
    s_out,
    r_out,
    s_ag,
    r_ag,
    s_fw,
    r_fw,
    s_mid,
    r_mid,
    s_part,
    r_part,
    s_ret,
    r_ret,
):
    s, t = lax.axis_index("sp"), lax.axis_index("tp")
    rows, col = stream_s.shape
    width = col * n_tp
    cap = outgoing.shape[0] // n_sp
    groups = n_sp // 2
    span = 2 * cap
    chip = s // 2
    sp_others = [lax.rem(s + d, n_sp) for d in range(1, n_sp)]
    beside = t + 1 - 2 * lax.rem(t, 2)
    across = t + 2 - 4 * (t // 2)
    corner = 3 - t
    peers = [beside, across, corner]
    far = len(peers)

    def at(start, size):
        return pl.ds(pl.multiple_of(start, size), size)

    own = at(t * col, col)
    pairs = (
        (ow_hbm, ow_ref),
        (res_hbm.at[:, own], res_ref),
        (gate_hbm, gate_w),
        (up_hbm, up_w),
        (down_hbm, down_w),
    )
    loads = [pltpu.make_async_copy(a, b, w_sem.at[i]) for i, (a, b) in enumerate(pairs)]
    for load in loads:
        load.start()

    def remote(src, dst, send, recv, device):
        return pltpu.make_async_remote_copy(
            src_ref=src,
            dst_ref=dst,
            send_sem=send,
            recv_sem=recv,
            device_id=device,
            device_id_type=MESH,
        )

    def term_copy(d):
        return remote(terms.at[d], terms_in.at[d], s_term.at[d], r_term.at[d], {"tp": peers[d]})

    def sum_copy(d):
        return remote(sums, sums_in.at[d], s_sum.at[d], r_sum.at[d], {"tp": peers[d]})

    def out_copy(dst, src):
        return remote(
            outgoing.at[at(dst * cap, cap)],
            arrived.at[t, at(src * cap, cap)],
            s_out.at[dst],
            r_out.at[src],
            {"sp": dst},
        )

    def ag_copy(d, g, owner):
        piece = arrived.at[owner, at(g * span, span)]
        return remote(piece, piece, s_ag.at[d, g], r_ag.at[d, g], {"tp": peers[d]})

    def fw_copy(d, g, owner):
        piece = arrived.at[owner, at((2 * g + d) * cap, cap)]
        return remote(piece, piece, s_fw.at[d, g], r_fw.at[d, g], {"tp": peers[1 - d]})

    def mid_copy(d, g):
        return remote(
            parts.at[3, at((2 * g + d) * cap, cap)],
            mid.at[d, at(g * cap, cap)],
            s_mid.at[d, g],
            r_mid.at[d, g],
            {"tp": peers[d]},
        )

    def part_copy(d, half, g):
        here = at((2 * g + half) * cap, cap)
        return remote(
            parts.at[1 + d, here],
            parts_in.at[d, here],
            s_part.at[d, half, g],
            r_part.at[d, half, g],
            {"tp": peers[d]},
        )

    def ret_copy(dst, src):
        return remote(
            ret.at[at(dst * cap, cap)],
            ret_in.at[at(src * cap, cap)],
            s_ret.at[dst],
            r_ret.at[src],
            {"sp": dst},
        )

    greet([{"tp": p} for p in peers] + [{"sp": p} for p in sp_others])
    attention_kernel(
        n_sp, q_ref, k_ref, v_ref, pack, recv, made, back, send1, recv1, send2, recv2
    )
    loads[0].wait()
    loads[1].wait()
    mixed = back[...].reshape(n_sp * HD, rows).T
    for d in (2, 0, 1):
        terms[d] = dot_f32(mixed, ow_ref[:, at(peers[d] * col, col)]).astype(BF16)
        term_copy(d).start()
    attended = dot_f32(mixed, ow_ref[:, own]).astype(BF16).astype(F32)

    routes = routes_ref[...].astype(F32)
    turned = [jnp.broadcast_to(routes[k : k + 1, :], (128, rows)).T for k in range(2)]
    lane = lax.broadcasted_iota(jnp.int32, (rows, 128), 1).astype(F32)
    named = [(column == lane).astype(F32) for column in turned]
    row_of = lax.broadcasted_iota(jnp.int32, (rows, rows), 0)
    col_of = lax.broadcasted_iota(jnp.int32, (rows, rows), 1)
    earlier = (col_of < row_of).astype(F32).astype(BF16)
    before = dot_f32(earlier, (named[0] + named[1]).astype(BF16))
    tgt_cols, tgt_rows = [], []
    for k in range(2):
        slot = jnp.sum(before * named[k], axis=1, keepdims=True)
        target = turned[k] * float(cap) + slot
        tgt_cols.append(target[:, 0:1].astype(jnp.int32))
        tgt_rows.append(target.T[0:1, :].astype(jnp.int32))

    for d in (0, 1, 2):
        term_copy(d).wait_recv()
        attended = attended + terms_in[d].astype(F32)
    attended = attended.astype(BF16).astype(F32)
    stream = (res_ref[...].astype(F32) + attended).astype(BF16).astype(F32)
    stream_s[...] = stream
    squares = jnp.sum(stream * stream, axis=1, keepdims=True)
    sums[...] = jnp.broadcast_to(squares, (rows, 128)).T[0:8, :]
    for d in range(far):
        sum_copy(d).start()
    square_row = sums[0:1, :]
    for d in range(far):
        sum_copy(d).wait_recv()
        square_row = square_row + sums_in[d, 0:1, :]
    squares = jnp.broadcast_to(square_row, (128, rows)).T[:, 0:1]
    normed = (
        stream * lax.rsqrt(squares * (1.0 / width) + epsilon) * gain_ref[0:1, own]
    ).astype(BF16)
    slot_in = lax.broadcasted_iota(jnp.int32, (cap, rows), 0)

    def dispatch(e):
        slots = slot_in + e * cap
        pick = ((tgt_rows[0] == slots) | (tgt_rows[1] == slots)).astype(F32).astype(BF16)
        return dot_f32(pick, normed).astype(BF16)

    arrived[t, at(s * cap, cap), :] = dispatch(s)
    partner = s + 1 - 2 * lax.rem(s, 2)
    targets = [partner]
    for k in range(1, groups):
        there = lax.rem(chip + groups - k, groups)
        targets += [2 * there, 2 * there + 1]
    for dst in targets:
        outgoing[at(dst * cap, cap), :] = dispatch(dst)
        out_copy(dst, s).start()

    def group_of(k):
        return lax.rem(chip + k, groups)

    def relay(k):
        g = group_of(k)
        for core in range(2):
            src = 2 * g + core

            @pl.when(src != s)
            def _():
                out_copy(src, src).wait_recv()

        for d in range(2):
            ag_copy(d, g, t).start()

    def forward(k):
        g = group_of(k)
        for d in range(2):
            ag_copy(d, g, peers[d]).wait_recv()
            fw_copy(d, g, peers[d]).start()

    def compute(k):
        g = group_of(k)
        for d in range(2):
            fw_copy(d, g, corner).wait_recv()
        ff = gate_w.shape[1]
        tile = min(256, ff)
        here = at(g * span, span)

        def hidden_tile(i, carry):
            lanes = at(i * tile, tile)
            gate_act = jnp.zeros((span, tile), F32)
            up_act = jnp.zeros((span, tile), F32)
            for c in range(n_tp):
                x = arrived[c, here, :]
                gate_act = gate_act + dot_f32(x, gate_w[c * col : (c + 1) * col, lanes])
                up_act = up_act + dot_f32(x, up_w[c * col : (c + 1) * col, lanes])
            act = gate_act / (1.0 + jnp.exp(-gate_act)) * up_act
            hidden[:, lanes] = act.astype(BF16)
            return carry

        lax.fori_loop(0, ff // tile, hidden_tile, 0)

        def part(place, owner):
            parts[place, here, :] = dot_f32(
                hidden[...], down_w[:, at(owner * col, col)]
            ).astype(BF16)

        part(3, corner)
        mid_copy(0, g).start()
        mid_copy(1, g).start()
        part(1, beside)
        part_copy(0, 0, g).start()
        part(2, across)
        part_copy(1, 1, g).start()
        part(0, t)

    def add(k):
        g = group_of(k)
        for d in range(2):
            mid_copy(d, g).wait_recv()
            here = at((2 * g + d) * cap, cap)
            both = parts[2 - d, here, :].astype(F32) + mid[d, at(g * cap, cap), :].astype(F32)
            parts[2 - d, here, :] = both.astype(BF16)
            part_copy(1 - d, d, g).start()

    def finish(k):
        g = group_of(k)
        here = at(g * span, span)
        for d in range(2):
            for half in range(2):
                part_copy(d, half, g).wait_recv()
        total = parts[0, here, :].astype(F32) + parts_in[0, here, :].astype(F32)
        ret[here, :] = (total + parts_in[1, here, :].astype(F32)).astype(BF16)
        for core in range(2):
            src = 2 * g + core

            @pl.when(src != s)
            def _():
                ret_copy(src, s).start()

    relay(0)
    relay(1)
    forward(0)
    for load in loads[2:]:
        load.wait()

    def step(k, carry):
        @pl.when(k + 2 < groups)
        def _():
            relay(k + 2)

        compute(k)

        @pl.when(k + 1 < groups)
        def _():
            forward(k + 1)

        @pl.when(k > 0)
        def _():
            add(k - 1)

        @pl.when(k > 1)
        def _():
            finish(k - 2)

        return carry

    lax.fori_loop(0, groups, step, 0)
    add(groups - 1)
    finish(groups - 2)
    finish(groups - 1)
    ret_in[at(s * cap, cap), :] = ret[at(s * cap, cap), :]
    for dst in sp_others:
        ret_copy(dst, dst).wait_recv()
    slots = lax.broadcasted_iota(jnp.int32, (rows, n_sp * cap), 1)
    gap = jnp.broadcast_to(scores_ref[1:2, :] - scores_ref[0:1, :], (128, rows)).T[:, 0:1]
    shares = (1.0 / (1.0 + jnp.exp(gap)), 1.0 / (1.0 + jnp.exp(-gap)))
    total = jnp.zeros((rows, col), F32)
    for k in range(2):
        pick = (tgt_cols[k] == slots).astype(F32).astype(BF16)
        total = total + dot_f32(pick, ret_in[...]) * shares[k]
    out_ref[...] = (stream_s[...] + total).astype(BF16)
    for d in range(far):
        term_copy(d).wait_send()
        sum_copy(d).wait_send()
    for dst in sp_others:
        out_copy(dst, s).wait_send()
        ret_copy(dst, s).wait_send()

    def drain(g, carry):
        for d in range(2):
            ag_copy(d, g, t).wait_send()
            fw_copy(d, g, peers[d]).wait_send()
            mid_copy(d, g).wait_send()
            for half in range(2):
                part_copy(d, half, g).wait_send()
        return carry

    lax.fori_loop(0, groups, drain, 0)


def fused_shards(
    n_sp,
    n_tp,
    residual_in,
    queries,
    keys,
    values,
    out_weight,
    norm_gain,
    expert_routes,
    route_scores,
    gate_weight,
    up_weight,
    down_weight,
):
    rows, width = residual_in.shape
    col = width // n_tp
    cap = 4 * rows // n_sp
    slots = n_sp * cap
    ff = gate_weight.shape[2]
    anywhere = pl.BlockSpec(memory_space=pl.ANY)
    dma = pltpu.SemaphoreType.DMA
    far = n_tp - 1
    groups = n_sp // 2
    held = [
        (n_sp, 3 * HD, rows),
        (n_sp, 3 * HD, rows),
        (n_sp, HD, rows),
        (n_sp, HD, rows),
    ]
    moved = [
        (out_weight.shape, BF16),
        ((rows, col), BF16),
        ((width, ff), BF16),
        ((width, ff), BF16),
        ((ff, width), BF16),
        ((far, rows, col), BF16),
        ((far, rows, col), BF16),
        ((8, rows), F32),
        ((far, 8, rows), F32),
        ((slots, col), BF16),
        ((n_tp, slots, col), BF16),
        ((2 * cap, ff), BF16),
        ((n_tp, slots, col), BF16),
        ((2, slots // 2, col), BF16),
        ((2, slots, col), BF16),
        ((slots, col), BF16),
        ((slots, col), BF16),
        ((rows, col), F32),
    ]
    counts = [(5,)] + [(far,)] * 4 + [(n_sp,)] * 2 + [(2, groups)] * 6
    counts += [(2, 2, groups)] * 2 + [(n_sp,)] * 2
    return pl.pallas_call(
        functools.partial(expert_kernel, n_sp, n_tp),
        out_shape=jax.ShapeDtypeStruct((rows, col), BF16),
        in_specs=[VM] * 6 + [anywhere] * 5,
        out_specs=VM,
        scratch_shapes=[pltpu.VMEM(shape, BF16) for shape in held]
        + [dma((n_sp,))] * 4
        + [pltpu.VMEM(shape, kind) for shape, kind in moved]
        + [dma(count) for count in counts],
        compiler_params=pltpu.CompilerParams(
            collective_id=0, has_side_effects=True, vmem_limit_bytes=60 * 1024 * 1024
        ),
    )(
        queries,
        keys,
        values,
        expert_routes.T,
        route_scores.T,
        norm_gain.reshape(1, width),
        out_weight,
        residual_in,
        gate_weight[0],
        up_weight[0],
        down_weight[0],
    )


def solution(mesh):
    in_specs = (
        P("sp", None),
        P("sp", "tp"),
        P("sp", "tp"),
        P("sp", "tp"),
        P("tp", None),
        P(),
        P("sp", None),
        P("sp", None),
        P("sp", None, "tp"),
        P("sp", None, "tp"),
        P("sp", "tp", None),
    )
    out_specs = P("sp", "tp")
    n_sp, n_tp = mesh.shape["sp"], mesh.shape["tp"]

    def body(*args):
        heads = args[1].shape[1] // HD
        if heads == n_sp and n_tp == 4 and n_sp % 4 == 0 and n_sp <= 128:
            return fused_shards(n_sp, n_tp, *args)
        return shards(*args)

    return jax.shard_map(body, mesh=mesh, in_specs=in_specs, out_specs=out_specs, check_vma=False)
```
